512 devices in a mesh: sp: 64 (over z, y), tp: 8 (over x, core).
Axes of the slice: x: 4, y: 4, z: 16, core: 2. Of those that a mesh axis runs over, the one named last changes fastest.
Arguments:
- latent: bfloat16 [16384, 2048], P(('sp', 'tp')), may hold values from -3 to 3
- context: bfloat16 [1024, 2048], P('sp'), may hold values from -6 to 6
- condition: float32 [2048], replicated, may hold values from -6 to 6
- ctx_cond: float32 [2048], replicated, may hold values from -6 to 6
- norm_gain: float32 [2048], replicated, may hold values from 0.1 to 1.9
- w_shift: bfloat16 [2048, 2048], P('sp', 'tp'), may hold values from -0.25 to 0.25
- w_scale: bfloat16 [2048, 2048], P('sp', 'tp'), may hold values from -0.25 to 0.25
- w_gate: bfloat16 [2048, 2048], P('sp', 'tp'), may hold values from -0.25 to 0.25
- w_query: bfloat16 [2048, 2048], P(None, 'tp'), may hold values from -0.125 to 0.125
- w_key: bfloat16 [2048, 2048], P(None, 'tp'), may hold values from -0.125 to 0.125
- w_value: bfloat16 [2048, 2048], P(None, 'tp'), may hold values from -0.125 to 0.125
- w_out: bfloat16 [2048, 2048], P('tp'), may hold values from -0.125 to 0.125
- rel_bias: float32 [16, 15, 31], replicated, may hold values from 2 to 250
Outputs:
- updated: bfloat16 [16384, 2048], P(('sp', 'tp'))
The draws below stay inside these ranges and needn't reach their ends.
All inputs are finite; a program needn't handle non-finite values.
Results may differ from the reference program's by a relative error of at most 0.015.
Values may be sent and summed in bfloat16 or wider, within the bound.
A program may use at most 64 MiB of HBM per device.

```python
import jax
import jax.numpy as jnp
import numpy as np
from jax import lax

D = 2048
HEADS = 16
HEAD_DIM = 128
GRID_W = 32
WIN_H = 8
WIN_W = 16
CTX = 1024
TOKENS = 16384
N_TP = 8


def draw_rel_bias(key, part):
    drawn = jax.random.uniform(key, (HEADS, 2 * WIN_H - 1, 2 * WIN_W - 1), jnp.float32, 2.0, 4.0)
    return drawn


def steps_of(stream_key, dims, split, low, largest):
    loudness, own = 1.0, jax.random.fold_in(stream_key, 6)
    for axis_at, blocks in split:
        steps = jnp.exp(jax.random.uniform(jax.random.fold_in(own, axis_at), (blocks,), jnp.float32, low / len(split), largest / len(split)))
        loudness = loudness * jnp.repeat(steps, dims[axis_at] // blocks).reshape([-1 if axis == axis_at else 1 for axis in range(len(dims))])
    return loudness


def noise(own_key, dims, deviation, limit, shards=(), held_as=jnp.bfloat16):
    level = steps_of(own_key, dims, shards, -0.22, 0.18) if shards else 1.0
    values = jax.random.normal(own_key, dims, jnp.float32) * deviation * level
    return jnp.minimum(jnp.maximum(values, -limit), limit).astype(held_as)


def setup_inputs(seed: int = 0) -> dict:
    splits = jax.random.split(jax.random.key(seed), 14)
    return {
        "latent": noise(splits[0], (TOKENS, D), 0.5, 3.0, ((0, 512),)),
        "context": noise(splits[1], (CTX, D), 1.0, 6.0, ((0, 64),)),
        "condition": noise(splits[2], (D,), 1.0, 6.0, (), jnp.float32),
        "ctx_cond": noise(splits[3], (D,), 1.0, 6.0, (), jnp.float32),
        "norm_gain": jnp.clip(1.0 + 0.18 * jax.random.normal(splits[4], (D,), jnp.float32), 0.1, 1.9),
        "w_shift": noise(splits[5], (D, D), (D // 4) ** -0.5, 0.25, ((0, 64), (1, 8))),
        "w_scale": noise(splits[6], (D, D), (D // 4) ** -0.5, 0.25, ((0, 64), (1, 8))),
        "w_gate": noise(splits[7], (D, D), (D // 4) ** -0.5, 0.25, ((0, 64), (1, 8))),
        "w_query": noise(splits[8], (D, D), D ** -0.5, 0.125, ((1, 8),)),
        "w_key": noise(splits[9], (D, D), D ** -0.5, 0.125, ((1, 8),)),
        "w_value": noise(splits[10], (D, D), D ** -0.5, 0.125, ((1, 8),)),
        "w_out": noise(splits[11], (D, D), D ** -0.5, 0.125, ((0, 8),)),
        "rel_bias": draw_rel_bias(jax.random.fold_in(splits[13], 71), 0),
    }


NORM_EPS = 1e-06
NEG_BIG = -1e+30

def rms_mod(block, norm_gain, shifts, scales):
    block = block.astype(jnp.float32)
    normed = block * lax.rsqrt(lax.optimization_barrier(jnp.mean(block * block, axis=-1, keepdims=True)) + NORM_EPS) * norm_gain
    return (normed * (1.0 + scales) + shifts).astype(jnp.bfloat16)

def project(block, weight):
    return jnp.dot(block, weight, preferred_element_type=jnp.float32).astype(jnp.bfloat16)

def geometry(total_rows):
    row_ids = np.arange(total_rows)
    starts = np.clip(row_ids - WIN_H // 2, 0, total_rows - WIN_H)
    row_index = starts[:, None] + np.arange(WIN_H)[None, :]
    row_off = row_index - row_ids[:, None] + WIN_H - 1
    col_ids = np.arange(GRID_W)
    col_start = np.clip(col_ids - WIN_W // 2, 0, GRID_W - WIN_W)
    col_in = (col_ids[None, :] >= col_start[:, None]) & (col_ids[None, :] < col_start[:, None] + WIN_W)
    col_off = np.clip(col_ids[None, :] - col_ids[:, None], 1 - WIN_W, WIN_W - 1) + WIN_W - 1
    return (row_index, row_off, col_in, col_off)

def reference(latent, context, condition, ctx_cond, norm_gain, w_shift, w_scale, w_gate, w_query, w_key, w_value, w_out, rel_bias):
    activated = jax.nn.silu(jnp.stack([condition, ctx_cond])).astype(jnp.bfloat16)
    shifts = jnp.dot(activated, w_shift, preferred_element_type=jnp.float32)
    scales = jnp.dot(activated, w_scale, preferred_element_type=jnp.float32)
    gate_vec = jnp.dot(activated[:1], w_gate, preferred_element_type=jnp.float32)[0]
    normed = rms_mod(latent, norm_gain, shifts[0], scales[0])
    ctx_normed = rms_mod(context, norm_gain, shifts[1], scales[1])
    queries = project(normed, w_query)
    lat_keys = project(normed, w_key)
    lat_values = project(normed, w_value)
    ctx_keys = project(ctx_normed, w_key)
    ctx_values = project(ctx_normed, w_value)
    total_rows = latent.shape[0] // GRID_W
    row_index, row_off, col_in, col_off = geometry(total_rows)
    inv_scale = HEAD_DIM ** (-0.5)

    def grid_heads(array):
        return jnp.transpose(array.reshape(total_rows, GRID_W, HEADS, HEAD_DIM), (2, 0, 1, 3))

    def ctx_heads(array):
        return jnp.transpose(array.reshape(-1, HEADS, HEAD_DIM), (1, 0, 2))

    def per_head(operands):
        query_head, key_head, value_head, ctx_key_head, ctx_value_head, bias_table = operands
        query_f = query_head.astype(jnp.float32)
        key_win = key_head[row_index].astype(jnp.float32)
        val_win = value_head[row_index].astype(jnp.float32)
        bias_win = bias_table[row_off[:, None, :, None], col_off[None, :, None, :]]
        scores_win = jnp.einsum('rqd,rkwd->rqkw', query_f, key_win) * inv_scale + bias_win
        scores_win = jnp.where(col_in[None, :, None, :], scores_win, NEG_BIG)
        scores_ctx = jnp.einsum('rqd,cd->rqc', query_f, ctx_key_head.astype(jnp.float32)) * inv_scale
        row_max = jnp.maximum(lax.optimization_barrier(jnp.max(scores_win, axis=(2, 3))), lax.optimization_barrier(jnp.max(scores_ctx, axis=2)))
        exp_win = jnp.exp(scores_win - row_max[:, :, None, None])
        exp_ctx = jnp.exp(scores_ctx - row_max[:, :, None])
        row_total = lax.optimization_barrier(jnp.sum(exp_win, axis=(2, 3))) + lax.optimization_barrier(jnp.sum(exp_ctx, axis=2))
        probs_win = (exp_win / row_total[:, :, None, None]).astype(jnp.bfloat16)
        probs_ctx = (exp_ctx / row_total[:, :, None]).astype(jnp.bfloat16)
        mixed_head = jnp.einsum('rqkw,rkwd->rqd', probs_win.astype(jnp.float32), val_win)
        mixed_head = mixed_head + jnp.einsum('rqc,cd->rqd', probs_ctx.astype(jnp.float32), ctx_value_head.astype(jnp.float32))
        return mixed_head.astype(jnp.bfloat16)
    attended = lax.map(per_head, (grid_heads(queries), grid_heads(lat_keys), grid_heads(lat_values), ctx_heads(ctx_keys), ctx_heads(ctx_values), rel_bias))
    attended = jnp.transpose(attended, (1, 2, 0, 3)).reshape(-1, HEADS * HEAD_DIM)
    head_cols = HEADS // N_TP * HEAD_DIM
    branch = jnp.zeros(latent.shape, jnp.float32)
    for group_idx in range(N_TP):
        low = group_idx * head_cols
        part_sum = jnp.dot(attended[:, low:low + head_cols], w_out[low:low + head_cols], preferred_element_type=jnp.float32).astype(jnp.bfloat16)
        part_sum = lax.optimization_barrier(part_sum)
        branch = branch + part_sum.astype(jnp.float32)
    return (latent.astype(jnp.float32) + gate_vec * branch).astype(jnp.bfloat16)
```

```python
import jax
import jax.numpy as jnp
from jax import lax
from jax.experimental import pallas as pl
from jax.experimental.pallas import tpu as pltpu
from jax.sharding import Mesh
from jax.sharding import PartitionSpec as P

HEADS = 16
HEAD_DIM = 128
GRID_W = 32
WIN_H = 8
WIN_W = 16
NORM_EPS = 1e-06
NEG_BIG = -1e30
NZ, NY, NX, NC = 16, 4, 4, 2
NSP = NZ * NY
GRID_R = 512
D = 2048
F32 = jnp.float32
BF16 = jnp.bfloat16
A_OFFS = (4, -3, 3, -2, 2, -1, 1)
B_OFFS = (4, -4)


def dot(a, b):
    return jnp.dot(a, b, preferred_element_type=F32)


def dot_t(a, b):
    return lax.dot_general(a, b, (((1,), (1,)), ((), ())), preferred_element_type=F32)


def silu(v):
    return v / (1.0 + jnp.exp(-v))


def kernel(
    lat_hbm, ctx_hbm, cond_hbm, cctx_hbm, gain_hbm, wsh_hbm, wsc_hbm, wga_hbm,
    wq_hbm, wk_hbm, wv_hbm, wo_hbm, rb_hbm, out_ref,
    latb, ctxb, condv, gainv, wmod, wq, wk, wv, wob, rbv,
    pbuf, abuf, sbuf, bbuf, tbuf, cbuf, mod,
    gmv, shv, gatev, rl, rc, xn, xc, qbuf, kbuf, vbuf, kvc, rolled, bias,
    att, attp, obuf, rbuf,
    ld, snd, a_r, b_r, c_r, m_r, lat_r, ring_r, part_r, wo_r, kv_r, att_r, out_r,
):
    z, y, x, c = (lax.axis_index(name) for name in ("z", "y", "x", "c"))
    t = x * 2 + c
    sp = z * NY + y
    pc = 1 - c
    sends = []

    def zz(d):
        return lax.rem(z + (NZ + d), NZ)

    def yy(d):
        return lax.rem(y + (NY + d), NY)

    def xx(d):
        return lax.rem(x + (NX + d), NX)

    def spd(d):
        other = lax.rem(sp + (NSP + d), NSP)
        return (other // NY, lax.rem(other, NY), x, c)

    def rcopy(src, dst, ssem, rsem, dev):
        return pltpu.make_async_remote_copy(
            src_ref=src, dst_ref=dst, send_sem=ssem, recv_sem=rsem,
            device_id=dev, device_id_type=pl.DeviceIdType.MESH,
        )

    def send(src, dst, rsem, dev):
        copy = rcopy(src, dst, snd.at[len(sends)], rsem, dev)
        copy.start()
        sends.append(copy)

    partner = (z, y, x, pc)

    def arrive(dst, rsem):
        rcopy(dst, dst, snd.at[0], rsem, partner).wait_recv()

    barrier = pltpu.get_barrier_semaphore()
    greet = [(zz(d), y, x, c) for d in (1, 2, 3, 4, -1, -2, -3, -4)]
    greet += [(z, yy(d), x, c) for d in (1, 2, 3)]
    greet += [
        (z, y, xx(dx), c if dc == 0 else pc) for dx in range(4) for dc in range(2) if dx or dc
    ]
    greet += [spd(1), spd(-1)]
    for dev in greet:
        pl.semaphore_signal(barrier, inc=1, device_id=dev, device_id_type=pl.DeviceIdType.MESH)

    wmod[...] = jnp.zeros_like(wmod)
    mine = pl.ds(pl.multiple_of(y * 32, 32), 32)
    loads = [
        (cond_hbm, condv.at[0]),
        (cctx_hbm, condv.at[1]),
        (wsh_hbm, wmod.at[0, mine, :]),
        (wsc_hbm, wmod.at[1, mine, :]),
        (wga_hbm, wmod.at[2, mine, :]),
        (lat_hbm, latb.at[4 + t]),
        (ctx_hbm.at[:, pl.ds(0, 1024)], ctxb.at[z, 0]),
        (ctx_hbm.at[:, pl.ds(1024, 1024)], ctxb.at[z, 1]),
        (rb_hbm.at[pl.ds(2 * t, 2)], rbv),
        (wo_hbm, wob.at[c]),
        (gain_hbm, gainv),
        (wk_hbm, wk),
        (wv_hbm, wv),
        (wq_hbm, wq),
    ]
    local = [pltpu.make_async_copy(s, d, ld.at[i]) for i, (s, d) in enumerate(loads)]
    for copy in local:
        copy.start()

    for i in range(5):
        local[i].wait()
    lane = lax.broadcasted_iota(jnp.int32, (8, 128), 1)
    row = lax.broadcasted_iota(jnp.int32, (8, 128), 0)
    keep = (lane >= y * 32) & (lane < y * 32 + 32)
    a0 = jnp.where(keep, silu(condv[0, pl.ds(z, 1), :]), 0.0)
    a1 = jnp.where(keep, silu(condv[1, pl.ds(z, 1), :]), 0.0)
    total = None
    for i in range(3):
        lhs = jnp.where(row == 2 * i, a0, 0.0)
        if i < 2:
            lhs = jnp.where(row == 2 * i + 1, a1, lhs)
        term = dot(lhs.astype(BF16), wmod[i])
        total = term if total is None else total + term
    pbuf[0:8, :] = total[:, :128]
    pbuf[8:16, :] = total[:, 128:]
    for i in range(5, 8):
        local[i].wait()
    pl.semaphore_wait(barrier, len(greet))

    for k, d in enumerate(A_OFFS):
        send(pbuf, abuf.at[k], a_r.at[k], (zz(d), y, x, c))

    def ring(slot, d):
        send(ctxb.at[slot, c], ctxb.at[slot, c], ring_r.at[slot], (zz(d), y, x, c))

    def to_partner_ctx(slot):
        send(ctxb.at[slot, c], ctxb.at[slot, c], part_r.at[slot], partner)

    def lat_send(slot, dev):
        send(latb.at[slot], latb.at[slot], lat_r.at[slot], dev)

    own_slot = 4 + t
    halo_slot = lax.rem(t + 12, 16)
    for d in (2, -2, 1, -1):
        ring(z, d)
    to_prev = x < 2
    spn = lax.rem(sp + jnp.where(to_prev, NSP - 1, 1), NSP)
    send(
        latb.at[own_slot], latb.at[halo_slot], lat_r.at[halo_slot],
        (spn // NY, lax.rem(spn, NY), x, c),
    )

    def lat_out(slot):
        for dx in (2, 1, 3):
            lat_send(slot, (z, y, xx(dx), c))
        lat_send(slot, partner)

    lat_out(own_slot)

    def ring_in(d):
        slot = zz(-d)
        arrive(ctxb.at[slot, c], ring_r.at[slot])
        return slot

    def ring_step(d):
        for sign in (1, -1):
            if sign == -1 and d == 8:
                continue
            slot = ring_in(sign * d)
            if d in (2, 4, 6):
                if not (sign == -1 and d == 6):
                    ring(slot, 2 * sign)
                ring(slot, sign)
            to_partner_ctx(slot)

    local[8].wait()
    row32 = lax.broadcasted_iota(jnp.int32, (32, 128), 0)
    lane32 = lax.broadcasted_iota(jnp.int32, (32, 128), 1)
    c2 = lax.rem(lane32, 32)
    b0 = jnp.clip(row32 - WIN_W // 2, 0, GRID_W - WIN_W)
    col_in = (c2 >= b0) & (c2 < b0 + WIN_W)
    quarter = lane32 // 32

    def bias_head(h, carry):
        def roll_e(e, inner):
            line = jnp.broadcast_to(rbv[h, pl.ds(e, 1), :], (32, 128))
            for k in range(4):
                rolled[e, k] = pltpu.roll(line, (32 * k + 113) % 128, 1, stride=1, stride_axis=0)
            return inner

        lax.fori_loop(0, 15, roll_e, 0)
        for i in range(8):
            first = sp * 8
            start = jnp.clip(first + i - WIN_H // 2, 0, GRID_R - WIN_H) - first + 4
            for q in range(4):
                tile = jnp.full((32, 128), NEG_BIG, F32)
                for k in range(4):
                    e = 4 * q + k - i + 3
                    if 0 <= e < 15:
                        tile = jnp.where(quarter == k, rolled[e, k], tile)
                j = 4 * q + quarter
                ok = col_in & (j >= start) & (j < start + WIN_H)
                bias[h, i % 2, (i // 2) * 32 : (i // 2) * 32 + 32, q * 128 : q * 128 + 128] = (
                    jnp.where(ok, tile, NEG_BIG)
                )
        return carry

    lax.fori_loop(0, 2, bias_head, 0)

    ring_step(1)
    ring_step(2)

    for k in range(7):
        arrive(abuf.at[k], a_r.at[k])
    part = pbuf[...]
    for k in range(7):
        part = part + abuf[k]
    sbuf[...] = part
    for k, d in enumerate(B_OFFS):
        send(sbuf, bbuf.at[k], b_r.at[k], (zz(d), y, x, c))

    arrive(latb.at[halo_slot], lat_r.at[halo_slot])
    lat_out(halo_slot)
    local[9].wait()
    send(wob.at[c], wob.at[c], wo_r, partner)

    ring_step(3)
    ring_step(4)

    for k in range(2):
        arrive(bbuf.at[k], b_r.at[k])
    tbuf[...] = bbuf[0] + bbuf[1]
    for k in range(3):
        send(tbuf, cbuf.at[k], c_r.at[k], (z, yy(k + 1), x, c))

    def lat_in(slot):
        arrive(latb.at[slot], lat_r.at[slot])

    for dx in (1, 3, 2):
        slot = 4 + xx(dx) * 2 + c
        lat_in(slot)
        lat_send(slot, partner)
    ring_step(5)
    ring_step(6)

    for k in range(3):
        arrive(cbuf.at[k], c_r.at[k])
    mod[t] = tbuf[...] + cbuf[0] + cbuf[1] + cbuf[2]
    for dx in (2, 1, 3, 0):
        for dc in range(2):
            if dx or dc:
                send(mod.at[t], mod.at[t], m_r.at[t], (z, y, xx(dx), c if dc == 0 else pc))

    for dx in (1, 3, 2):
        slot = lax.rem(xx(dx) * 2 + c + 12, 16)
        lat_in(slot)
        lat_send(slot, partner)
    ring_step(7)
    ring_step(8)

    for d in range(1, NZ):
        slot = zz(d)
        arrive(ctxb.at[slot, pc], part_r.at[slot])
    for dx in range(4):
        other = xx(dx) * 2 + pc
        lat_in(4 + other)
        lat_in(lax.rem(other + 12, 16))

    def ctx_tile(g, j):
        block = ctxb[pl.ds(8 * g, 8), j // 8, :, (j % 8) * 128 : (j % 8) * 128 + 128]
        return block.reshape(128, 128).astype(F32)

    def lat_tile(g, j):
        return latb[pl.ds(4 * g, 4), :, j * 128 : j * 128 + 128].reshape(128, 128).astype(F32)

    def stats(tile_of, dest, count):
        def step(g, carry):
            acc = jnp.zeros((128, 128), F32)
            for j in range(16):
                tile = tile_of(g, j)
                acc = acc + tile * tile
            mean = jnp.sum(acc, axis=1, keepdims=True) * (1.0 / D)
            dest[pl.ds(pl.multiple_of(128 * g, 128), 128), :] = jnp.broadcast_to(
                lax.rsqrt(mean + NORM_EPS), (128, 128)
            )
            return carry

        lax.fori_loop(0, count, step, 0)

    stats(ctx_tile, rc, 2)
    stats(lat_tile, rl, 4)
    local[10].wait()
    for dx in range(4):
        for dc in range(2):
            if dx or dc:
                slot = xx(dx) * 2 + (c if dc == 0 else pc)
                arrive(mod.at[slot], m_r.at[slot])
    for j in range(16):
        low = (j % 2) * 8
        for which in range(2):
            gmv[which, j : j + 1, :] = gainv[j : j + 1, :] * (
                1.0 + mod[j // 2, low + 2 + which : low + 3 + which, :]
            )
            shv[which, j : j + 1, :] = mod[j // 2, low + which : low + which + 1, :]
        gatev[j : j + 1, :] = mod[j // 2, low + 4 : low + 5, :]

    def normed(tile_of, scale, which, dest, count):
        def step(g, carry):
            rows = pl.ds(pl.multiple_of(128 * g, 128), 128)
            inv = scale[rows, :]
            for j in range(16):
                value = tile_of(g, j) * inv * gmv[which, j : j + 1, :] + shv[which, j : j + 1, :]
                dest[rows, j * 128 : j * 128 + 128] = value.astype(BF16)
            return carry

        lax.fori_loop(0, count, step, 0)

    normed(ctx_tile, rc, 1, xc, 2)
    local[11].wait()
    local[12].wait()
    kvc[y, :, 0:256] = dot(xc[...], wk[...]).astype(BF16)
    kvc[y, :, 256:512] = dot(xc[...], wv[...]).astype(BF16)

    def kv_send(slot, half, d, k):
        ref = kvc.at[slot, pl.ds(128 * half, 128), :]
        send(ref, ref, kv_r.at[k], (z, yy(d), x, c))

    def kv_in(d, half, k):
        arrive(kvc.at[yy(d), pl.ds(128 * half, 128), :], kv_r.at[k])

    kv_send(y, 0, 1, 0)
    kv_send(y, 1, -1, 1)
    kv_send(y, 1, 1, 2)
    kv_send(y, 0, -1, 3)

    normed(lat_tile, rl, 0, xn, 4)
    kv_in(-1, 0, 0)
    kv_send(yy(-1), 0, 1, 4)
    kv_in(1, 1, 1)
    kv_send(yy(1), 1, -1, 5)

    def project(g, carry):
        rows = pl.ds(pl.multiple_of(256 * g, 256), 256)
        kbuf[rows, :] = dot(xn[rows, :], wk[...]).astype(BF16)
        vbuf[rows, :] = dot(xn[rows, :], wv[...]).astype(BF16)
        return carry

    lax.fori_loop(0, 2, project, 0)
    local[13].wait()
    queries = dot(xn[128:384, :], wq[...]).astype(BF16)
    for i in range(8):
        qbuf[i % 2, (i // 2) * 32 : (i // 2) * 32 + 32, :] = queries[i * 32 : i * 32 + 32, :]

    kv_in(-1, 1, 2)
    kv_in(1, 0, 3)
    kv_in(2, 0, 4)
    kv_in(2, 1, 5)

    inv_scale = HEAD_DIM**-0.5

    def attend(par):
        for h in range(2):
            cols = slice(h * 128, h * 128 + 128)
            vcols = slice(256 + h * 128, 256 + h * 128 + 128)
            q = qbuf[par, :, cols]
            s_win = dot_t(q, kbuf[:, cols]) * inv_scale + bias[h, par]
            s_ctx = dot_t(q, kvc[:, :, cols].reshape(1024, 128)) * inv_scale
            top = jnp.maximum(
                jnp.max(s_win, axis=1, keepdims=True), jnp.max(s_ctx, axis=1, keepdims=True)
            )
            e_win = jnp.exp(s_win - top)
            e_ctx = jnp.exp(s_ctx - top)
            norm = jnp.sum(e_win, axis=1, keepdims=True) + jnp.sum(e_ctx, axis=1, keepdims=True)
            mixed = dot(e_win.astype(BF16), vbuf[:, cols]) + dot(
                e_ctx.astype(BF16), kvc[:, :, vcols].reshape(1024, 128)
            )
            att[par, :, cols] = (mixed / norm).astype(BF16)

    attend(pc)
    send(att.at[pc], attp, att_r, partner)
    attend(c)
    arrive(attp, att_r)
    arrive(wob.at[pc], wo_r)

    def out_cols(n, carry):
        cols = pl.ds(pl.multiple_of(512 * n, 512), 512)
        value = dot(att[c], wob[c, :, cols]) + dot(attp[...], wob[pc, :, cols])
        obuf[:, :, cols] = value.astype(BF16).reshape(4, 32, 512)
        return carry

    lax.fori_loop(0, 4, out_cols, 0)
    for dx in (2, 1, 3):
        send(obuf.at[xx(dx)], rbuf.at[dx - 1], out_r.at[dx - 1], (z, y, xx(dx), c))
    for dx in (1, 3, 2):
        arrive(rbuf.at[dx - 1], out_r.at[dx - 1])
    for j in range(16):
        cols = slice(j * 128, j * 128 + 128)
        branch = obuf[x, :, cols].astype(F32)
        for k in range(3):
            branch = branch + rbuf[k, :, cols].astype(F32)
        out_ref[:, cols] = (
            latb[own_slot, :, cols].astype(F32) + gatev[j : j + 1, :] * branch
        ).astype(BF16)
    for copy in sends:
        copy.wait_send()


N_SENDS = 7 + 4 + 1 + 4 + 11 + 15 + 2 + 4 + 1 + 3 + 3 + 7 + 3 + 6 + 1 + 3


def on_device(
    latent, context, condition, ctx_cond, norm_gain, w_shift, w_scale, w_gate,
    w_query, w_key, w_value, w_out, rel_bias,
):
    vm = pltpu.VMEM
    dma = pltpu.SemaphoreType.DMA
    bias_rows = jnp.pad(rel_bias, ((0, 0), (0, 1), (0, 97)))
    return pl.pallas_call(
        kernel,
        out_shape=jax.ShapeDtypeStruct((32, D), BF16),
        in_specs=[pl.BlockSpec(memory_space=pl.ANY)] * 13,
        out_specs=pl.BlockSpec(memory_space=pltpu.VMEM),
        scratch_shapes=[
            vm((16, 32, D), BF16),
            vm((16, 2, 16, 1024), BF16),
            vm((2, 16, 128), F32),
            vm((16, 128), F32),
            vm((3, 128, 256), BF16),
            vm((D, 256), BF16),
            vm((D, 256), BF16),
            vm((D, 256), BF16),
            vm((2, 256, D), BF16),
            vm((2, 16, 128), F32),
            vm((16, 128), F32),
            vm((7, 16, 128), F32),
            vm((16, 128), F32),
            vm((2, 16, 128), F32),
            vm((16, 128), F32),
            vm((3, 16, 128), F32),
            vm((8, 16, 128), F32),
            vm((2, 16, 128), F32),
            vm((2, 16, 128), F32),
            vm((16, 128), F32),
            vm((512, 128), F32),
            vm((256, 128), F32),
            vm((512, D), BF16),
            vm((256, D), BF16),
            vm((2, 128, 256), BF16),
            vm((512, 256), BF16),
            vm((512, 256), BF16),
            vm((4, 256, 512), BF16),
            vm((15, 4, 32, 128), F32),
            vm((2, 2, 128, 512), F32),
            vm((2, 128, 256), BF16),
            vm((128, 256), BF16),
            vm((4, 32, D), BF16),
            vm((3, 32, D), BF16),
            dma((14,)),
            dma((N_SENDS,)),
            dma((7,)),
            dma((2,)),
            dma((3,)),
            dma((8,)),
            dma((16,)),
            dma((16,)),
            dma((16,)),
            dma(()),
            dma((6,)),
            dma(()),
            dma((3,)),
        ],
        compiler_params=pltpu.CompilerParams(
            collective_id=0, has_side_effects=True, vmem_limit_bytes=56 * 1024 * 1024
        ),
        name="whole_step",
    )(
        latent, context, condition.reshape(16, 128), ctx_cond.reshape(16, 128),
        norm_gain.reshape(16, 128), w_shift, w_scale, w_gate, w_query, w_key, w_value, w_out,
        bias_rows,
    )


def solution(mesh):
    torus = Mesh(mesh.devices.reshape(NZ, NY, NX, NC), ("z", "y", "x", "c"))
    sp, tp = ("z", "y"), ("x", "c")
    return jax.shard_map(
        on_device,
        mesh=torus,
        in_specs=(
            P((*sp, *tp), None),
            P(sp, None),
            P(),
            P(),
            P(),
            P(sp, tp),
            P(sp, tp),
            P(sp, tp),
            P(None, tp),
            P(None, tp),
            P(None, tp),
            P(tp, None),
            P(),
        ),
        out_specs=P((*sp, *tp), None),
        check_vma=False,
    )
```

```python
import jax
import jax.numpy as jnp
from jax import lax
from jax.experimental import pallas as pl
from jax.experimental.pallas import tpu as pltpu
from jax.sharding import Mesh
from jax.sharding import PartitionSpec as P

HEADS = 16
HEAD_DIM = 128
GRID_W = 32
WIN_H = 8
WIN_W = 16
NORM_EPS = 1e-06
NEG_BIG = -1e30
NZ, NY, NX, NC = 16, 4, 4, 2
NSP = NZ * NY
GRID_R = 512
D = 2048
F32 = jnp.float32
BF16 = jnp.bfloat16
A_OFFS = (4, -3, 3, -2, 2, -1, 1)
B_OFFS = (4, -4)
GROUPS = ((0, 1), (1, 5), (5, 9), (9, 13), (13, 16))


def dot(a, b):
    return jnp.dot(a, b, preferred_element_type=F32)


def dot_t(a, b):
    return lax.dot_general(a, b, (((1,), (1,)), ((), ())), preferred_element_type=F32)


def silu(v):
    return v / (1.0 + jnp.exp(-v))


def kernel(
    lat_hbm, ctx_hbm, cond_hbm, cctx_hbm, gain_hbm, wsh_hbm, wsc_hbm, wga_hbm,
    wq_hbm, wk_hbm, wv_hbm, wo_hbm, rb_hbm, out_ref,
    latb, ctxb, condv, gainv, wmod, wq, wk, wv, wob, rbv,
    pbuf, abuf, sbuf, bbuf, tbuf, cbuf, mod,
    gmv, shv, gatev, rl, rc, xn, xc, qbuf, kbuf, vbuf, kvc, rolled, bias,
    att, attp, obuf, rbuf,
    ld, snd, a_r, b_r, c_r, m_r, lat_r, ring_r, own_r, y_r, y_p, far_r, far_p,
    wo_r, att_r, out_r,
):
    z, y, x, c = (lax.axis_index(name) for name in ("z", "y", "x", "c"))
    t = x * 2 + c
    sp = z * NY + y
    pc = 1 - c
    sends = []

    def zz(d):
        return lax.rem(z + (NZ + d), NZ)

    def yy(d):
        return lax.rem(y + (NY + d), NY)

    def xx(d):
        return lax.rem(x + (NX + d), NX)

    def spd(d):
        other = lax.rem(sp + (NSP + d), NSP)
        return (other // NY, lax.rem(other, NY), x, c)

    def rcopy(src, dst, ssem, rsem, dev):
        return pltpu.make_async_remote_copy(
            src_ref=src, dst_ref=dst, send_sem=ssem, recv_sem=rsem,
            device_id=dev, device_id_type=pl.DeviceIdType.MESH,
        )

    def send(src, dst, rsem, dev):
        copy = rcopy(src, dst, snd.at[len(sends)], rsem, dev)
        copy.start()
        sends.append(copy)

    partner = (z, y, x, pc)

    def arrive(dst, rsem):
        rcopy(dst, dst, snd.at[0], rsem, partner).wait_recv()

    scope = []

    def phase(name):
        if scope:
            scope.pop().__exit__(None, None, None)
        if name:
            scope.append(jax.named_scope(name))
            scope[0].__enter__()

    phase("greet")
    barrier = pltpu.get_barrier_semaphore()
    greet = [(zz(d), y, x, c) for d in (1, 2, 3, 4, -1, -2, -3, -4)]
    greet += [(z, yy(d), x, c) for d in (1, 2, 3)]
    greet += [
        (z, y, xx(dx), c if dc == 0 else pc) for dx in range(4) for dc in range(2) if dx or dc
    ]
    greet += [spd(1), spd(-1)]
    for dev in greet:
        pl.semaphore_signal(barrier, inc=1, device_id=dev, device_id_type=pl.DeviceIdType.MESH)

    wmod[...] = jnp.zeros_like(wmod)
    mine = pl.ds(pl.multiple_of(y * 32, 32), 32)
    loads = [
        (cond_hbm, condv.at[0]),
        (cctx_hbm, condv.at[1]),
        (wsh_hbm, wmod.at[0, mine, :]),
        (wsc_hbm, wmod.at[1, mine, :]),
        (wga_hbm, wmod.at[2, mine, :]),
        (lat_hbm, latb.at[4 + t]),
        (ctx_hbm.at[:, pl.ds(0, 1024)], ctxb.at[0, 0, 0]),
        (ctx_hbm.at[:, pl.ds(1024, 1024)], ctxb.at[0, 1, 0]),
        (rb_hbm.at[pl.ds(2 * t, 2)], rbv),
        (wo_hbm, wob.at[c]),
        (gain_hbm, gainv),
        (wk_hbm, wk),
        (wv_hbm, wv),
        (wq_hbm, wq),
    ]
    local = [pltpu.make_async_copy(s, d, ld.at[i]) for i, (s, d) in enumerate(loads)]
    for copy in local:
        copy.start()

    phase("mod_load")
    for i in range(5):
        local[i].wait()
    phase("mod_term")
    lane = lax.broadcasted_iota(jnp.int32, (8, 128), 1)
    row = lax.broadcasted_iota(jnp.int32, (8, 128), 0)
    keep = (lane >= y * 32) & (lane < y * 32 + 32)
    a0 = jnp.where(keep, silu(condv[0, pl.ds(z, 1), :]), 0.0)
    a1 = jnp.where(keep, silu(condv[1, pl.ds(z, 1), :]), 0.0)
    total = None
    for i in range(3):
        lhs = jnp.where(row == 2 * i, a0, 0.0)
        if i < 2:
            lhs = jnp.where(row == 2 * i + 1, a1, lhs)
        term = dot(lhs.astype(BF16), wmod[i])
        total = term if total is None else total + term
    pbuf[0:8, :] = total[:, :128]
    pbuf[8:16, :] = total[:, 128:]
    phase("wait_barrier")
    for i in range(5, 8):
        local[i].wait()
    pl.semaphore_wait(barrier, len(greet))

    phase("send_first")
    for k in range(3):
        send(pbuf, cbuf.at[k], c_r.at[k], (z, yy(k + 1), x, c))

    def piece(r, half, lo, hi):
        return ctxb.at[r, half, pl.ds(lo, hi - lo)]

    def ring(slot, sub, d):
        near = (slot + 1) // 2
        far = near + abs(d)
        to = 2 * far - 1 if d > 0 else 2 * far
        cols = pl.ds(512 * sub, 512)
        send(
            ctxb.at[0, c, slot, :, cols], ctxb.at[0, c, to, :, cols],
            ring_r.at[to, sub], (zz(d), y, x, c),
        )

    def ring_group(g):
        lo, hi = GROUPS[g]
        for sub in range(2):
            cols = pl.ds(512 * sub, 512)
            for slot in sorted(range(lo, hi), key=lambda s: ((s + 1) // 2) % 2):
                arrive(ctxb.at[0, c, slot, :, cols], ring_r.at[slot, sub])
                near, sign = (slot + 1) // 2, 1 if slot % 2 else -1
                if near in (2, 4, 6):
                    if not (sign == -1 and near == 6):
                        ring(slot, sub, 2 * sign)
                    ring(slot, sub, sign)
        y_out(g)
        own = piece(0, c, lo, hi)
        send(own, own, own_r.at[g], partner)

    def y_out(g):
        lo, hi = GROUPS[g]
        for k in range(2):
            send(
                piece(0, c, lo, hi), piece(1 + k, c, lo, hi), y_r.at[k, g],
                (z, yy(1 if k == 0 else -1), x, c),
            )

    def halves(g):
        lo, hi = GROUPS[g]
        mid = (lo + hi + (g == 0)) // 2
        return ((lo, mid), (mid, hi))

    def y_in(g):
        lo, hi = GROUPS[g]
        for k in range(2):
            got = piece(1 + k, c, lo, hi)
            arrive(got, y_r.at[k, g])
            first, last = halves(g)[k]
            if last > first:
                send(
                    piece(1 + k, c, first, last), piece(3, c, first, last), far_r.at[k, g],
                    (z, yy(1 if k == 0 else -1), x, c),
                )
            send(got, got, y_p.at[k, g], partner)

    def far_in(g):
        for k in range(2):
            first, last = halves(g)[k]
            if last > first:
                got = piece(3, c, first, last)
                arrive(got, far_r.at[k, g])
                send(got, got, far_p.at[k, g], partner)

    def own_ready():
        for g in range(1, 5):
            arrive(piece(0, pc, *GROUPS[g]), own_r.at[g])

    def y_ready(k):
        for g in range(5):
            arrive(piece(1 + k, pc, *GROUPS[g]), y_p.at[k, g])

    def far_ready():
        for g in range(5):
            for k in range(2):
                first, last = halves(g)[k]
                if last > first:
                    arrive(piece(3, pc, first, last), far_p.at[k, g])

    def lat_send(slot, dev):
        send(latb.at[slot], latb.at[slot], lat_r.at[slot], dev)

    own_slot = 4 + t
    halo_slot = lax.rem(t + 12, 16)
    for sub in range(2):
        for d in (2, -2, 1, -1):
            ring(0, sub, d)
    y_out(0)
    to_prev = x < 2
    spn = lax.rem(sp + jnp.where(to_prev, NSP - 1, 1), NSP)
    send(
        latb.at[own_slot], latb.at[halo_slot], lat_r.at[halo_slot],
        (spn // NY, lax.rem(spn, NY), x, c),
    )

    def lat_out(slot):
        for dx in (2, 1, 3):
            lat_send(slot, (z, y, xx(dx), c))
        lat_send(slot, partner)

    lat_out(own_slot)

    phase("bias")
    local[8].wait()
    row32 = lax.broadcasted_iota(jnp.int32, (32, 128), 0)
    lane32 = lax.broadcasted_iota(jnp.int32, (32, 128), 1)
    c2 = lax.rem(lane32, 32)
    b0 = jnp.clip(row32 - WIN_W // 2, 0, GRID_W - WIN_W)
    col_in = (c2 >= b0) & (c2 < b0 + WIN_W)
    quarter = lane32 // 32

    def bias_head(h, carry):
        def roll_e(e, inner):
            line = jnp.broadcast_to(rbv[h, pl.ds(e, 1), :], (32, 128))
            for k in range(4):
                rolled[e, k] = pltpu.roll(line, (32 * k + 113) % 128, 1, stride=1, stride_axis=0)
            return inner

        lax.fori_loop(0, 15, roll_e, 0)
        for i in range(8):
            first = sp * 8
            start = jnp.clip(first + i - WIN_H // 2, 0, GRID_R - WIN_H) - first + 4
            for q in range(4):
                tile = jnp.full((32, 128), NEG_BIG, F32)
                for k in range(4):
                    e = 4 * q + k - i + 3
                    if 0 <= e < 15:
                        tile = jnp.where(quarter == k, rolled[e, k], tile)
                j = 4 * q + quarter
                ok = col_in & (j >= start) & (j < start + WIN_H)
                bias[h, i // 2, (i % 2) * 32 : (i % 2) * 32 + 32, q * 128 : q * 128 + 128] = (
                    jnp.where(ok, tile, NEG_BIG)
                )
        return carry

    lax.fori_loop(0, 2, bias_head, 0)

    def lat_in(slot):
        arrive(latb.at[slot], lat_r.at[slot])

    phase("mod_y")
    for k in range(3):
        arrive(cbuf.at[k], c_r.at[k])
    sbuf[...] = (pbuf[...] + cbuf[0] + cbuf[1] + cbuf[2]).astype(BF16)
    for k, d in enumerate(A_OFFS):
        send(sbuf, abuf.at[k], a_r.at[k], (zz(d), y, x, c))

    phase("ring1")
    ring_group(1)
    phase("halo")
    lat_in(halo_slot)
    lat_out(halo_slot)
    local[9].wait()
    send(wob.at[c], wob.at[c], wo_r, partner)
    phase("y0")
    y_in(0)

    phase("mod_a")
    for k in range(7):
        arrive(abuf.at[k], a_r.at[k])
    part = sbuf[...].astype(F32)
    for k in range(7):
        part = part + abuf[k].astype(F32)
    tbuf[...] = part
    for k, d in enumerate(B_OFFS):
        send(tbuf, bbuf.at[k], b_r.at[k], (zz(d), y, x, c))

    phase("lat_own")
    for dx in (1, 3, 2):
        slot = 4 + xx(dx) * 2 + c
        lat_in(slot)
        lat_send(slot, partner)
    phase("ring2")
    ring_group(2)
    phase("y1")
    y_in(1)
    far_in(0)

    phase("mod_b")
    for k in range(2):
        arrive(bbuf.at[k], b_r.at[k])
    mod[t] = bbuf[0] + bbuf[1]
    for dx in (2, 1, 3, 0):
        for dc in range(2):
            if dx or dc:
                send(mod.at[t], mod.at[t], m_r.at[t], (z, y, xx(dx), c if dc == 0 else pc))

    phase("ring3")
    ring_group(3)
    phase("lat_halo")
    for dx in (1, 3, 2):
        slot = lax.rem(xx(dx) * 2 + c + 12, 16)
        lat_in(slot)
        lat_send(slot, partner)
    phase("y2")
    y_in(2)
    far_in(1)

    phase("lat_parts")
    for dx in range(4):
        other = xx(dx) * 2 + pc
        lat_in(4 + other)
        lat_in(lax.rem(other + 12, 16))

    def ctx_tile(g, j):
        block = ctxb[
            g // 2, j // 8, pl.ds(8 * lax.rem(g, 2), 8), :, (j % 8) * 128 : (j % 8) * 128 + 128
        ]
        return block.reshape(128, 128).astype(F32)

    def lat_tile(g, j):
        return latb[pl.ds(4 * g, 4), :, j * 128 : j * 128 + 128].reshape(128, 128).astype(F32)

    def stats(tile_of, dest, first, count):
        def step(g, carry):
            acc = jnp.zeros((128, 128), F32)
            for j in range(16):
                tile = tile_of(g, j)
                acc = acc + tile * tile
            mean = jnp.sum(acc, axis=1, keepdims=True) * (1.0 / D)
            dest[pl.ds(pl.multiple_of(128 * g, 128), 128), :] = jnp.broadcast_to(
                lax.rsqrt(mean + NORM_EPS), (128, 128)
            )
            return carry

        lax.fori_loop(first, first + count, step, 0)

    phase("lat_stats")
    stats(lat_tile, rl, 0, 4)
    phase("ring4")
    ring_group(4)
    phase("mod_gather")
    local[10].wait()
    for dx in range(4):
        for dc in range(2):
            if dx or dc:
                slot = xx(dx) * 2 + (c if dc == 0 else pc)
                arrive(mod.at[slot], m_r.at[slot])
    phase("mod_rows")
    for j in range(16):
        low = (j % 2) * 8
        for which in range(2):
            gmv[which, j : j + 1, :] = gainv[j : j + 1, :] * (
                1.0 + mod[j // 2, low + 2 + which : low + 3 + which, :]
            )
            shv[which, j : j + 1, :] = mod[j // 2, low + which : low + which + 1, :]
        gatev[j : j + 1, :] = mod[j // 2, low + 4 : low + 5, :]

    def normed(tile_of, scale, which, dest, first, count):
        def step(g, carry):
            rows = pl.ds(pl.multiple_of(128 * g, 128), 128)
            to = pl.ds(pl.multiple_of(128 * (g - first), 128), 128)
            inv = scale[rows, :]
            for j in range(16):
                value = tile_of(g, j) * inv * gmv[which, j : j + 1, :] + shv[which, j : j + 1, :]
                dest[to, j * 128 : j * 128 + 128] = value.astype(BF16)
            return carry

        lax.fori_loop(first, first + count, step, 0)

    def project(g, carry):
        rows = pl.ds(pl.multiple_of(256 * g, 256), 256)
        kbuf[rows, :] = dot(xn[rows, :], wk[...]).astype(BF16)
        vbuf[rows, :] = dot(xn[rows, :], wv[...]).astype(BF16)
        return carry

    def context(r):
        stats(ctx_tile, rc, 2 * r, 2)
        normed(ctx_tile, rc, 1, xc, 2 * r, 2)
        kvc[r, :, 0:256] = dot(xc[...], wk[...]).astype(BF16)
        kvc[r, :, 256:512] = dot(xc[...], wv[...]).astype(BF16)

    phase("y3")
    y_in(3)
    far_in(2)
    for i in (11, 12, 13):
        local[i].wait()
    phase("lat_norm")
    normed(lat_tile, rl, 0, xn, 0, 4)
    phase("lat_proj")
    lax.fori_loop(0, 2, project, 0)
    phase("lat_q")
    queries = dot(xn[128:384, :], wq[...]).astype(BF16)
    for i in range(8):
        qbuf[i // 2, (i % 2) * 32 : (i % 2) * 32 + 32, :] = queries[i * 32 : i * 32 + 32, :]
    phase("own_wait")
    own_ready()
    phase("ctx0")
    context(0)
    phase("y4")
    y_in(4)
    far_in(3)
    phase("y_wait0")
    y_ready(0)
    phase("ctx1")
    context(1)
    phase("far4")
    far_in(4)
    phase("y_wait1")
    y_ready(1)
    phase("ctx2")
    context(2)
    phase("far_wait")
    far_ready()
    phase("ctx3")
    context(3)
    phase("attend")

    inv_scale = HEAD_DIM**-0.5

    def attend(off):
        to = xx(off)
        for h in range(2):
            cols = slice(h * 128, h * 128 + 128)
            vcols = slice(256 + h * 128, 256 + h * 128 + 128)
            q = qbuf[to, :, cols]
            s_win = dot_t(q, kbuf[:, cols]) * inv_scale + bias[h, to]
            s_ctx = dot_t(q, kvc[:, :, cols].reshape(1024, 128)) * inv_scale
            top = jnp.maximum(
                jnp.max(s_win, axis=1, keepdims=True), jnp.max(s_ctx, axis=1, keepdims=True)
            )
            e_win = jnp.exp(s_win - top)
            e_ctx = jnp.exp(s_ctx - top)
            norm = jnp.sum(e_win, axis=1, keepdims=True) + jnp.sum(e_ctx, axis=1, keepdims=True)
            mixed = dot(e_win.astype(BF16), vbuf[:, cols]) + dot(
                e_ctx.astype(BF16), kvc[:, :, vcols].reshape(1024, 128)
            )
            att[to, :, :, cols] = (mixed / norm).astype(BF16).reshape(2, 32, 128)
        send(att.at[to, pc], attp.at[to], att_r.at[off], partner)

    def finish(off):
        to = xx(off)
        arrive(attp.at[to], att_r.at[off])
        mine_rows, other_rows = att[to, c], attp[to]

        def out_cols(n, carry):
            cols = pl.ds(pl.multiple_of(512 * n, 512), 512)
            value = dot(mine_rows, wob[c, :, cols]) + dot(other_rows, wob[pc, :, cols])
            obuf[to, :, cols] = value.astype(BF16)
            return carry

        lax.fori_loop(0, 4, out_cols, 0)
        if off:
            send(obuf.at[to], rbuf.at[off - 1], out_r.at[off - 1], (z, y, to, c))

    attend(2)
    arrive(wob.at[pc], wo_r)
    attend(1)
    phase("finish2")
    finish(2)
    phase("attend3")
    attend(3)
    phase("finish1")
    finish(1)
    phase("attend0")
    attend(0)
    phase("finish3")
    finish(3)
    phase("finish0")
    finish(0)
    phase("out_wait")
    for dx in (1, 3, 2):
        arrive(rbuf.at[dx - 1], out_r.at[dx - 1])
    phase("final")
    for j in range(16):
        cols = slice(j * 128, j * 128 + 128)
        branch = obuf[x, :, cols].astype(F32)
        for k in range(3):
            branch = branch + rbuf[k, :, cols].astype(F32)
        out_ref[:, cols] = (
            latb[own_slot, :, cols].astype(F32) + gatev[j : j + 1, :] * branch
        ).astype(BF16)
    phase("drain")
    for copy in sends:
        copy.wait_send()
    phase(None)


N_SENDS = 19 + 8 + 22 + 10 + 4 + 10 + 9 + 9 + 15 + 1 + 4 + 3


def on_device(
    latent, context, condition, ctx_cond, norm_gain, w_shift, w_scale, w_gate,
    w_query, w_key, w_value, w_out, rel_bias,
):
    vm = pltpu.VMEM
    dma = pltpu.SemaphoreType.DMA
    bias_rows = jnp.pad(rel_bias, ((0, 0), (0, 1), (0, 97)))
    return pl.pallas_call(
        kernel,
        out_shape=jax.ShapeDtypeStruct((32, D), BF16),
        in_specs=[pl.BlockSpec(memory_space=pl.ANY)] * 13,
        out_specs=pl.BlockSpec(memory_space=pltpu.VMEM),
        scratch_shapes=[
            vm((16, 32, D), BF16),
            vm((4, 2, 16, 16, 1024), BF16),
            vm((2, 16, 128), F32),
            vm((16, 128), F32),
            vm((3, 128, 256), BF16),
            vm((D, 256), BF16),
            vm((D, 256), BF16),
            vm((D, 256), BF16),
            vm((2, 256, D), BF16),
            vm((2, 16, 128), F32),
            vm((16, 128), F32),
            vm((7, 16, 128), BF16),
            vm((16, 128), BF16),
            vm((2, 16, 128), F32),
            vm((16, 128), F32),
            vm((3, 16, 128), F32),
            vm((8, 16, 128), F32),
            vm((2, 16, 128), F32),
            vm((2, 16, 128), F32),
            vm((16, 128), F32),
            vm((512, 128), F32),
            vm((1024, 128), F32),
            vm((512, D), BF16),
            vm((256, D), BF16),
            vm((4, 64, 256), BF16),
            vm((512, 256), BF16),
            vm((512, 256), BF16),
            vm((4, 256, 512), BF16),
            vm((15, 4, 32, 128), F32),
            vm((2, 4, 64, 512), F32),
            vm((4, 2, 32, 256), BF16),
            vm((4, 32, 256), BF16),
            vm((4, 32, D), BF16),
            vm((3, 32, D), BF16),
            dma((14,)),
            dma((N_SENDS,)),
            dma((7,)),
            dma((2,)),
            dma((3,)),
            dma((8,)),
            dma((16,)),
            dma((16, 2)),
            dma((5,)),
            dma((2, 5)),
            dma((2, 5)),
            dma((2, 5)),
            dma((2, 5)),
            dma(()),
            dma((4,)),
            dma((3,)),
        ],
        compiler_params=pltpu.CompilerParams(
            collective_id=0, has_side_effects=True, vmem_limit_bytes=56 * 1024 * 1024
        ),
        name="whole_step",
    )(
        latent, context, condition.reshape(16, 128), ctx_cond.reshape(16, 128),
        norm_gain.reshape(16, 128), w_shift, w_scale, w_gate, w_query, w_key, w_value, w_out,
        bias_rows,
    )


def solution(mesh):
    torus = Mesh(mesh.devices.reshape(NZ, NY, NX, NC), ("z", "y", "x", "c"))
    sp, tp = ("z", "y"), ("x", "c")
    return jax.shard_map(
        on_device,
        mesh=torus,
        in_specs=(
            P((*sp, *tp), None),
            P(sp, None),
            P(),
            P(),
            P(),
            P(sp, tp),
            P(sp, tp),
            P(sp, tp),
            P(None, tp),
            P(None, tp),
            P(None, tp),
            P(tp, None),
            P(),
        ),
        out_specs=P((*sp, *tp), None),
        check_vma=False,
    )
```

```python
import jax
import jax.numpy as jnp
from jax import lax
from jax.experimental import pallas as pl
from jax.experimental.pallas import tpu as pltpu
from jax.sharding import Mesh
from jax.sharding import PartitionSpec as P

HEADS = 16
HEAD_DIM = 128
GRID_W = 32
WIN_H = 8
WIN_W = 16
NORM_EPS = 1e-06
NEG_BIG = -1e30
NZ, NY, NX, NC = 16, 4, 4, 2
NSP = NZ * NY
GRID_R = 512
D = 2048
F32 = jnp.float32
BF16 = jnp.bfloat16
A_OFFS = (4, -3, 3, -2, 2, -1, 1)
B_OFFS = (4, -4)
GROUPS = ((0, 1), (1, 5), (5, 9), (9, 13), (13, 16))


def dot(a, b):
    return jnp.dot(a, b, preferred_element_type=F32)


def dot_t(a, b):
    return lax.dot_general(a, b, (((1,), (1,)), ((), ())), preferred_element_type=F32)


def silu(v):
    return v / (1.0 + jnp.exp(-v))


def kernel(
    lat_hbm, ctx_hbm, cond_hbm, cctx_hbm, gain_hbm, wsh_hbm, wsc_hbm, wga_hbm,
    wq_hbm, wk_hbm, wv_hbm, wo_hbm, rb_hbm, out_ref,
    latb, ctxb, condv, gainv, wmod, w3, wob, rbv,
    pbuf, abuf, sbuf, bbuf, tbuf, cbuf, mod,
    gmv, shv, gatev, rl, rc, xn, xc, qbuf, kbuf, vbuf, kvc, rolled, bias,
    att, attp, obuf, mbuf, ubuf, fin,
    ld, snd, mod_r, ring_r, own_r, y_r, y_p, far_r, far_p, lat_r, end_r,
):
    z, y, x, c = (lax.axis_index(name) for name in ("z", "y", "x", "c"))
    t = x * 2 + c
    sp = z * NY + y
    pc = 1 - c

    def zz(d):
        return lax.rem(z + (NZ + d), NZ)

    def yy(d):
        return lax.rem(y + (NY + d), NY)

    def xx(d):
        return lax.rem(x + (NX + d), NX)

    def spd(d):
        other = lax.rem(sp + (NSP + d), NSP)
        return (other // NY, lax.rem(other, NY), x, c)

    def send(src, dst, kind, rsem, dev):
        pltpu.make_async_remote_copy(
            src_ref=src, dst_ref=dst, send_sem=snd.at[kind], recv_sem=rsem,
            device_id=dev, device_id_type=pl.DeviceIdType.MESH,
        ).start()

    partner = (z, y, x, pc)
    left, right = (z, y, xx(-1), c), (z, y, xx(1), c)

    def wait(view, sem):
        pltpu.make_async_copy(view, view, sem).wait()

    scope = []

    def phase(name):
        if scope:
            scope.pop().__exit__(None, None, None)
        if name:
            scope.append(jax.named_scope(name))
            scope[0].__enter__()

    phase("greet")
    barrier = pltpu.get_barrier_semaphore()
    greet = [(zz(d), y, x, c) for d in (1, 2, 3, 4, -1, -2, -3, -4)]
    greet += [(z, yy(d), x, c) for d in (1, 2, 3)]
    greet += [
        (z, y, xx(dx), c if dc == 0 else pc) for dx in range(4) for dc in range(2) if dx or dc
    ]
    greet += [spd(1), spd(-1)]
    for dev in greet:
        pl.semaphore_signal(barrier, inc=1, device_id=dev, device_id_type=pl.DeviceIdType.MESH)

    wmod[...] = jnp.zeros_like(wmod)
    mine = pl.ds(pl.multiple_of(y * 32, 32), 32)
    loads = [
        (cond_hbm, condv.at[0], 0),
        (cctx_hbm, condv.at[1], 0),
        (wsh_hbm, wmod.at[0, mine, :], 1),
        (wsc_hbm, wmod.at[1, mine, :], 1),
        (wga_hbm, wmod.at[2, mine, :], 1),
        (lat_hbm, latb.at[4 + t], 2),
        (ctx_hbm.at[:, pl.ds(0, 1024)], ctxb.at[0, 0, 0], 3),
        (ctx_hbm.at[:, pl.ds(1024, 1024)], ctxb.at[0, 1, 0], 3),
        (rb_hbm, rbv, 4),
        (wo_hbm, wob.at[c], 5),
        (gain_hbm, gainv, 6),
        (wk_hbm, w3.at[0], 7),
        (wv_hbm, w3.at[1], 7),
        (wq_hbm, w3.at[2], 7),
    ]
    for src, dst, k in loads:
        pltpu.make_async_copy(src, dst, ld.at[k]).start()

    phase("mod_load")
    wait(condv, ld.at[0])
    wait(wmod.at[:, mine, :], ld.at[1])
    phase("mod_term")
    lane = lax.broadcasted_iota(jnp.int32, (8, 128), 1)
    row = lax.broadcasted_iota(jnp.int32, (8, 128), 0)
    keep = (lane >= y * 32) & (lane < y * 32 + 32)
    a0 = jnp.where(keep, silu(condv[0, pl.ds(z, 1), :]), 0.0)
    a1 = jnp.where(keep, silu(condv[1, pl.ds(z, 1), :]), 0.0)
    total = None
    for i in range(3):
        lhs = jnp.where(row == 2 * i, a0, 0.0)
        if i < 2:
            lhs = jnp.where(row == 2 * i + 1, a1, lhs)
        term = dot(lhs.astype(BF16), wmod[i])
        total = term if total is None else total + term
    pbuf[0:8, :] = total[:, :128]
    pbuf[8:16, :] = total[:, 128:]
    phase("wait_barrier")
    wait(latb.at[4 + t], ld.at[2])
    wait(ctxb.at[0, :, 0], ld.at[3])
    pl.semaphore_wait(barrier, len(greet))

    phase("send_first")
    for k in range(3):
        send(pbuf, cbuf.at[k], 0, mod_r.at[0], (z, yy(k + 1), x, c))

    def piece(r, half, lo, hi):
        return ctxb.at[r, half, pl.ds(lo, hi - lo)]

    def ring(slot, sub, d):
        far = (slot + 1) // 2 + abs(d)
        to = 2 * far - 1 if d > 0 else 2 * far
        cols = pl.ds(512 * sub, 512)
        send(
            ctxb.at[0, c, slot, :, cols], ctxb.at[0, c, to, :, cols],
            2, ring_r.at[far - 1, sub], (zz(d), y, x, c),
        )

    def ring_in(near, sub):
        lo, hi = 2 * near - 1, min(2 * near + 1, 16)
        wait(ctxb.at[0, c, pl.ds(lo, hi - lo), :, pl.ds(512 * sub, 512)], ring_r.at[near - 1, sub])

    def ring_group(g):
        near = 2 * g
        for sub in range(2):
            ring_in(near, sub)
            if g < 4:
                ring(2 * near - 1, sub, 2)
                if g < 3:
                    ring(2 * near, sub, -2)
        if g < 4:
            for sub in range(2):
                ring(2 * near - 1, sub, 1)
                ring(2 * near, sub, -1)
        for sub in range(2):
            ring_in(near - 1, sub)
        y_out(g)
        own = piece(0, c, *GROUPS[g])
        send(own, own, 4, own_r.at[g // 3], partner)

    def y_out(g):
        for k in range(2):
            send(
                piece(0, c, *GROUPS[g]), piece(1 + k, c, *GROUPS[g]), 3, y_r.at[g],
                (z, yy(1 if k == 0 else -1), x, c),
            )

    def y_in(g):
        lo, hi = GROUPS[g]
        mid = (lo + hi + (g == 0)) // 2
        wait(ctxb.at[pl.ds(1, 2), c, pl.ds(lo, hi - lo)], y_r.at[g])
        for k, (first, last) in enumerate(((lo, mid), (mid, hi))):
            if last > first:
                send(
                    piece(1 + k, c, first, last), piece(3, c, first, last), 6, far_r.at[g],
                    (z, yy(1 if k == 0 else -1), x, c),
                )
        for k in range(2):
            got = piece(1 + k, c, lo, hi)
            send(got, got, 5, y_p.at[g // 3], partner)

    def far_in(g):
        got = piece(3, c, *GROUPS[g])
        wait(got, far_r.at[g])
        send(got, got, 6, far_p.at[g // 3], partner)

    def lat_send(slot, rsem, dev):
        send(latb.at[slot], latb.at[slot], 7, rsem, dev)

    own_slot = 4 + t
    halo_slot = lax.rem(t + 12, 16)

    def slot_of(kind, dx, core):
        other = xx(dx) * 2 + core
        return 4 + other if kind == 0 else lax.rem(other + 12, 16)

    def lat_out(kind):
        slot = slot_of(kind, 0, c)
        lat_send(slot, lat_r.at[1 + kind], right)
        lat_send(slot, lat_r.at[1 + kind], left)
        lat_send(slot, lat_r.at[5], partner)

    def lat_near(kind):
        wait(latb.at[pl.ds(0, 2)], lat_r.at[1 + kind])
        for dx, lo, dev in ((-1, 0, right), (1, 16, left)):
            part = latb.at[slot_of(kind, dx, c), pl.ds(lo, 16)]
            send(part, part, 7, lat_r.at[3 + kind], dev)
        for dx in (-1, 1):
            lat_send(slot_of(kind, dx, c), lat_r.at[5], partner)

    def lat_far(kind):
        slot = slot_of(kind, 2, c)
        wait(latb.at[slot], lat_r.at[3 + kind])
        lat_send(slot, lat_r.at[5], partner)

    for d in (2, 1):
        for sub in range(2):
            for sign in (1, -1):
                ring(0, sub, d * sign)
    y_out(0)
    to_prev = x < 2
    spn = lax.rem(sp + jnp.where(to_prev, NSP - 1, 1), NSP)
    send(
        latb.at[own_slot], latb.at[halo_slot], 7, lat_r.at[0],
        (spn // NY, lax.rem(spn, NY), x, c),
    )
    lat_out(0)

    row32 = lax.broadcasted_iota(jnp.int32, (32, 128), 0)
    lane32 = lax.broadcasted_iota(jnp.int32, (32, 128), 1)
    c2 = lax.rem(lane32, 32)
    b0 = jnp.clip(row32 - WIN_W // 2, 0, GRID_W - WIN_W)
    col_in = (c2 >= b0) & (c2 < b0 + WIN_W)
    quarter = lane32 // 32

    def bias_head(h):
        def roll_e(e, inner):
            line = rbv[e, pl.ds(2 * t + h, 1), :]
            line = jnp.concatenate([line, jnp.zeros((1, 97), F32)], axis=1)
            line = jnp.broadcast_to(line, (32, 128))
            for k in range(4):
                rolled[e, k] = pltpu.roll(line, (32 * k + 113) % 128, 1, stride=1, stride_axis=0)
            return inner

        lax.fori_loop(0, 15, roll_e, 0)
        for i in range(8):
            first = sp * 8
            start = jnp.clip(first + i - WIN_H // 2, 0, GRID_R - WIN_H) - first + 4
            for q in range(4):
                tile = jnp.full((32, 128), NEG_BIG, F32)
                for k in range(4):
                    e = 4 * q + k - i + 3
                    if 0 <= e < 15:
                        tile = jnp.where(quarter == k, rolled[e, k], tile)
                j = 4 * q + quarter
                ok = col_in & (j >= start) & (j < start + WIN_H)
                bias[h, i % 2, (i // 2) * 32 : (i // 2) * 32 + 32, q * 128 : q * 128 + 128] = (
                    jnp.where(ok, tile, NEG_BIG)
                )

    phase("bias0")
    wait(rbv, ld.at[4])
    bias_head(0)

    phase("mod_y")
    wait(cbuf, mod_r.at[0])
    sbuf[...] = (pbuf[...] + cbuf[0] + cbuf[1] + cbuf[2]).astype(BF16)
    for k, d in enumerate(A_OFFS):
        send(sbuf, abuf.at[k], 1, mod_r.at[1], (zz(d), y, x, c))

    phase("ring1")
    ring_group(1)
    phase("halo")
    wait(latb.at[halo_slot], lat_r.at[0])
    lat_out(1)
    wait(wob.at[c], ld.at[5])
    send(wob.at[c], wob.at[c], 8, end_r.at[0], partner)
    phase("bias1")
    bias_head(1)
    phase("y0")
    y_in(0)
    phase("lat_own")
    lat_near(0)

    phase("mod_a")
    wait(abuf, mod_r.at[1])
    part = sbuf[...].astype(F32)
    for k in range(7):
        part = part + abuf[k].astype(F32)
    tbuf[...] = part
    for k, d in enumerate(B_OFFS):
        send(tbuf, bbuf.at[k], 0, mod_r.at[2], (zz(d), y, x, c))

    phase("ring2")
    ring_group(2)
    phase("y1")
    y_in(1)
    far_in(0)
    phase("lat_halo")
    lat_near(1)
    lat_far(0)

    phase("ring3")
    ring_group(3)
    phase("mod_b")
    wait(bbuf, mod_r.at[2])
    mod[t] = bbuf[0] + bbuf[1]
    for dx in (2, 1, 3, 0):
        for dc in range(2):
            if dx or dc:
                send(
                    mod.at[t], mod.at[t], 0, mod_r.at[3],
                    (z, y, xx(dx), c if dc == 0 else pc),
                )

    phase("y2")
    y_in(2)
    far_in(1)
    phase("lat_far")
    lat_far(1)

    def ctx_tile(g, j):
        block = ctxb[
            g // 2, j // 8, pl.ds(8 * lax.rem(g, 2), 8), :, (j % 8) * 128 : (j % 8) * 128 + 128
        ]
        return block.reshape(128, 128).astype(F32)

    def lat_tile(g, j):
        return latb[pl.ds(4 * g, 4), :, j * 128 : j * 128 + 128].reshape(128, 128).astype(F32)

    def stats(tile_of, dest, first, count, step_by=1):
        def step(i, carry):
            g = first + i * step_by
            acc = jnp.zeros((128, 128), F32)
            for j in range(16):
                tile = tile_of(g, j)
                acc = acc + tile * tile
            mean = jnp.sum(acc, axis=1, keepdims=True) * (1.0 / D)
            dest[pl.ds(pl.multiple_of(128 * g, 128), 128), :] = jnp.broadcast_to(
                lax.rsqrt(mean + NORM_EPS), (128, 128)
            )
            return carry

        lax.fori_loop(0, count, step, 0)

    phase("stats_ctx")
    wait(ctxb.at[0, pc, pl.ds(1, 8)], own_r.at[0])
    wait(ctxb.at[pl.ds(1, 2), pc, pl.ds(0, 9)], y_p.at[0])
    stats(ctx_tile, rc, 0, 3, 2)
    phase("ring4")
    ring_group(4)
    phase("lat_parts")
    wait(latb.at[pl.ds(0, 8)], lat_r.at[5])
    phase("stats_lat")
    stats(lat_tile, rl, 0, 4)
    phase("y3")
    y_in(3)
    far_in(2)
    phase("mod_gather")
    wait(gainv, ld.at[6])
    wait(w3, ld.at[7])
    wait(rl.at[pl.ds(0, 112)], mod_r.at[3])
    phase("mod_rows")
    for j in range(16):
        low = (j % 2) * 8
        for which in range(2):
            gmv[which, j : j + 1, :] = gainv[j : j + 1, :] * (
                1.0 + mod[j // 2, low + 2 + which : low + 3 + which, :]
            )
            shv[which, j : j + 1, :] = mod[j // 2, low + which : low + which + 1, :]
        gatev[j : j + 1, :] = mod[j // 2, low + 4 : low + 5, :]

    def normed(tile_of, scale, which, dest, first, count):
        def step(g, carry):
            rows = pl.ds(pl.multiple_of(128 * g, 128), 128)
            to = pl.ds(pl.multiple_of(128 * (g - first), 128), 128)
            inv = scale[rows, :]
            for j in range(16):
                value = tile_of(g, j) * inv * gmv[which, j : j + 1, :] + shv[which, j : j + 1, :]
                dest[to, j * 128 : j * 128 + 128] = value.astype(BF16)
            return carry

        lax.fori_loop(first, first + count, step, 0)

    def project(g, carry):
        rows = pl.ds(pl.multiple_of(256 * g, 256), 256)
        kbuf[rows, :] = dot(xn[rows, :], w3[0]).astype(BF16)
        vbuf[rows, :] = dot(xn[rows, :], w3[1]).astype(BF16)
        return carry

    def context(r):
        normed(ctx_tile, rc, 1, xc, 2 * r, 2)
        kvc[r, :, 0:256] = dot(xc[...], w3[0]).astype(BF16)
        kvc[r, :, 256:512] = dot(xc[...], w3[1]).astype(BF16)

    phase("lat_norm")
    normed(lat_tile, rl, 0, xn, 0, 4)
    phase("lat_proj")
    lax.fori_loop(0, 2, project, 0)
    phase("lat_q")
    queries = dot(xn[128:384, :], w3[2]).astype(BF16)
    for i in range(8):
        qbuf[i % 2, (i // 2) * 32 : (i // 2) * 32 + 32, :] = queries[i * 32 : i * 32 + 32, :]
    phase("y4")
    y_in(4)
    far_in(3)
    phase("own_wait")
    wait(ctxb.at[0, pc, pl.ds(9, 7)], own_r.at[1])
    phase("ctx0")
    stats(ctx_tile, rc, 1, 1)
    context(0)
    phase("y_wait")
    wait(ctxb.at[pl.ds(1, 2), pc, pl.ds(9, 7)], y_p.at[1])
    phase("ctx1")
    stats(ctx_tile, rc, 3, 2, 2)
    context(1)
    phase("far4")
    far_in(4)
    phase("ctx2")
    context(2)
    phase("far_wait")
    wait(ctxb.at[3, pc, pl.ds(0, 9)], far_p.at[0])
    wait(ctxb.at[3, pc, pl.ds(9, 7)], far_p.at[1])
    phase("ctx3")
    stats(ctx_tile, rc, 6, 2)
    context(3)

    inv_scale = HEAD_DIM**-0.5

    def attend(par):
        for h in range(2):
            cols = slice(h * 128, h * 128 + 128)
            vcols = slice(256 + h * 128, 256 + h * 128 + 128)
            q = qbuf[par, :, cols]
            s_win = dot_t(q, kbuf[:, cols]) * inv_scale + bias[h, par]
            s_ctx = dot_t(q, kvc[:, :, cols].reshape(1024, 128)) * inv_scale
            top = jnp.maximum(
                jnp.max(s_win, axis=1, keepdims=True), jnp.max(s_ctx, axis=1, keepdims=True)
            )
            e_win = jnp.exp(s_win - top)
            e_ctx = jnp.exp(s_ctx - top)
            norm = jnp.sum(e_win, axis=1, keepdims=True) + jnp.sum(e_ctx, axis=1, keepdims=True)
            mixed = dot(e_win.astype(BF16), vbuf[:, cols]) + dot(
                e_ctx.astype(BF16), kvc[:, :, vcols].reshape(1024, 128)
            )
            att[par, :, cols] = (mixed / norm).astype(BF16)

    phase("attend")
    attend(pc)
    send(att.at[pc], attp, 9, end_r.at[1], partner)
    attend(c)
    phase("att_wait")
    wait(wob.at[pc], end_r.at[0])
    wait(attp, end_r.at[1])

    def out_cols(n, carry):
        cols = pl.ds(pl.multiple_of(512 * n, 512), 512)
        value = dot(att[c], wob[c, :, cols]) + dot(attp[...], wob[pc, :, cols])
        obuf[:, :, cols] = value.astype(BF16).reshape(4, 32, 512)
        return carry

    low_cols, high_cols = pl.ds(0, 1024), pl.ds(1024, 1024)

    def give(dest, cols, to, dev):
        send(obuf.at[dest, :, cols], to, 10, end_r.at[4], dev)

    phase("out_low")
    lax.fori_loop(0, 2, out_cols, 0)
    send(obuf.at[xx(2), :, low_cols], mbuf.at[0], 10, end_r.at[2], right)
    give(xx(-1), low_cols, fin.at[1, :, low_cols], left)
    phase("out_high")
    lax.fori_loop(2, 4, out_cols, 0)
    send(obuf.at[xx(2), :, high_cols], mbuf.at[1], 10, end_r.at[3], left)
    give(xx(1), high_cols, fin.at[0, :, high_cols], right)
    phase("out_sum")
    for k, cols, dx, dev in ((0, low_cols, 1, right), (1, high_cols, -1, left)):
        wait(mbuf.at[k], end_r.at[2 + k])
        ubuf[k] = (obuf[xx(dx), :, cols].astype(F32) + mbuf[k].astype(F32)).astype(BF16)
        send(ubuf.at[k], fin.at[k, :, cols], 10, end_r.at[4], dev)
    phase("out_wait")
    wait(fin, end_r.at[4])
    phase("final")
    for j in range(16):
        cols = slice(j * 128, j * 128 + 128)
        branch = (
            obuf[x, :, cols].astype(F32) + fin[0, :, cols].astype(F32) + fin[1, :, cols].astype(F32)
        )
        out_ref[:, cols] = gatev[j : j + 1, :] * branch
    phase("drain")
    slots = ctxb.at[0, 0, pl.ds(1, 15)]
    for k, view in enumerate((
        rl.at[pl.ds(0, 192)], abuf, slots, ctxb.at[0], slots, ctxb.at[0], ctxb.at[0],
        latb.at[pl.ds(0, 15)], wob.at[0], attp, latb.at[pl.ds(0, 3)],
    )):
        wait(view, snd.at[k])
    phase(None)


def on_device(
    latent, context, condition, ctx_cond, norm_gain, w_shift, w_scale, w_gate,
    w_query, w_key, w_value, w_out, rel_bias,
):
    vm = pltpu.VMEM
    dma = pltpu.SemaphoreType.DMA
    delta = pl.pallas_call(
        kernel,
        out_shape=jax.ShapeDtypeStruct((32, D), F32),
        in_specs=[pl.BlockSpec(memory_space=pl.ANY)] * 13,
        out_specs=pl.BlockSpec(memory_space=pltpu.VMEM),
        scratch_shapes=[
            vm((16, 32, D), BF16),
            vm((4, 2, 16, 16, 1024), BF16),
            vm((2, 16, 128), F32),
            vm((16, 128), F32),
            vm((3, 128, 256), BF16),
            vm((3, D, 256), BF16),
            vm((2, 256, D), BF16),
            vm((15, 16, 31), F32),
            vm((16, 128), F32),
            vm((7, 16, 128), BF16),
            vm((16, 128), BF16),
            vm((2, 16, 128), F32),
            vm((16, 128), F32),
            vm((3, 16, 128), F32),
            vm((8, 16, 128), F32),
            vm((2, 16, 128), F32),
            vm((2, 16, 128), F32),
            vm((16, 128), F32),
            vm((512, 128), F32),
            vm((1024, 128), F32),
            vm((512, D), BF16),
            vm((256, D), BF16),
            vm((2, 128, 256), BF16),
            vm((512, 256), BF16),
            vm((512, 256), BF16),
            vm((4, 256, 512), BF16),
            vm((15, 4, 32, 128), F32),
            vm((2, 2, 128, 512), F32),
            vm((2, 128, 256), BF16),
            vm((128, 256), BF16),
            vm((4, 32, D), BF16),
            vm((2, 32, 1024), BF16),
            vm((2, 32, 1024), BF16),
            vm((2, 32, D), BF16),
            dma((8,)),
            dma((11,)),
            dma((4,)),
            dma((8, 2)),
            dma((2,)),
            dma((5,)),
            dma((2,)),
            dma((5,)),
            dma((2,)),
            dma((6,)),
            dma((5,)),
        ],
        compiler_params=pltpu.CompilerParams(
            collective_id=0, has_side_effects=True, vmem_limit_bytes=56 * 1024 * 1024
        ),
        name="whole_step",
    )(
        latent, context, condition.reshape(16, 128), ctx_cond.reshape(16, 128),
        norm_gain.reshape(16, 128), w_shift, w_scale, w_gate, w_query, w_key, w_value, w_out,
        jnp.transpose(rel_bias, (1, 0, 2)),
    )
    return (latent.astype(F32) + delta).astype(BF16)


def solution(mesh):
    torus = Mesh(mesh.devices.reshape(NZ, NY, NX, NC), ("z", "y", "x", "c"))
    sp, tp = ("z", "y"), ("x", "c")
    return jax.shard_map(
        on_device,
        mesh=torus,
        in_specs=(
            P((*sp, *tp), None),
            P(sp, None),
            P(),
            P(),
            P(),
            P(sp, tp),
            P(sp, tp),
            P(sp, tp),
            P(None, tp),
            P(None, tp),
            P(None, tp),
            P(tp, None),
            P(),
        ),
        out_specs=P((*sp, *tp), None),
        check_vma=False,
    )
```
